32 devices in a mesh: grp: 2 (over y), sp: 4 (over z), tp: 4 (over x, core).
Axes of the slice: x: 2, y: 2, z: 4, core: 2. Of those that a mesh axis runs over, the one named last changes fastest.
Arguments:
- queries: bfloat16 [8192, 1024], P(('grp', 'sp'), 'tp'), parts along dimension 0, may hold values from -6 to 6
- keys: bfloat16 [8192, 256], P(('grp', 'sp')), parts along dimension 0, may hold values from -6 to 6
- values: bfloat16 [8192, 256], P(('grp', 'sp')), parts along dimension 0, may hold values from -6 to 6
- query_gain: float32 [128], replicated, may hold values from 1.2 to 6, as said below
- key_gain: float32 [128], replicated, may hold values from 1.2 to 6, as said below
- out_weight: bfloat16 [1024, 2048], replicated, may hold values from -6 to 6
- residual_in: bfloat16 [8192, 2048], P(('grp', 'sp', 'tp')), parts along dimension 0, may hold values from -6 to 6
- norm_gain: float32 [2048], replicated, may hold values from 0.1 to 1.9
- gate_weight: bfloat16 [2048, 2816], P('sp', 'tp'), may hold values from -0.125 to 0.125
- up_weight: bfloat16 [2048, 2816], P('sp', 'tp'), may hold values from -0.125 to 0.125
- down_weight: bfloat16 [2816, 2048], P('tp', 'sp'), may hold values from -0.109375 to 0.109375
Outputs:
- layer_out: bfloat16 [8192, 2048], P(('grp', 'sp', 'tp')), parts along dimension 0
The draws below stay inside these ranges and needn't reach their ends.
There are 2 independent parts, one for each index of `grp`. The reference program is written for one: setup_inputs(seed, part) draws one part's arguments, and reference() takes and returns one part's arrays. A program takes and returns all parts, laid end to end along the dimension named above; an argument that names none is the same for every part. Nothing has to cross between parts.
Inputs may be any that keep to these rules, and one draw needn't show every extreme that they name: `query_gain`: positive gains. `key_gain`: positive gains.
All inputs are finite; a program needn't handle non-finite values.
Results may differ from the reference program's by a relative error of at most 0.015.
The reference program's roundings to bfloat16 on the way (of `query_rot`, `key_rot`, `probs`, `attended`, `normed` and `hidden`) count: a program that leaves them out, or rounds other values in their place, can miss the bound.
Values may be sent and summed in bfloat16 or wider, within the bound.
A program may use at most 128 MiB of HBM per device.

```python
import jax
import jax.numpy as jnp
from jax import lax

D = 2048
HQ = 8
KV = 2
HD = 128
FF = 2816
GRID_W = 64
TOK_DEV = 1024
TOKENS = 4096


def shared_draw(key):
    key_rows = jax.random.truncated_normal(jax.random.fold_in(key, 1), -6.0, 6.0, (TOKENS, KV * HD), jnp.float32)
    query_rows = jax.random.truncated_normal(jax.random.fold_in(key, 2), -6.0, 6.0, (TOKENS, HQ * HD), jnp.float32)
    return (query_rows, key_rows)


def draw_queries(key, part):
    return shared_draw(key)[0].astype(jnp.bfloat16)


def draw_keys(key, part):
    return shared_draw(key)[1].astype(jnp.bfloat16)


def draw_query_gain(key, part):
    return jax.random.uniform(jax.random.fold_in(key, 11), (HD,), jnp.float32, 1.2, 1.7)


def draw_key_gain(key, part):
    return jax.random.uniform(jax.random.fold_in(key, 12), (HD,), jnp.float32, 1.2, 1.7)


def block_levels(own_key, extent, pieces, low, largest):
    level = 1.0
    for dim, parts in pieces:
        draws = jax.random.uniform(jax.random.fold_in(jax.random.fold_in(own_key, 6), dim), (parts,), jnp.float32, low / len(pieces), largest / len(pieces))
        level = level * jnp.repeat(jnp.exp(draws), extent[dim] // parts).reshape((-1,) + (1,) * (len(extent) - 1 - dim))
    return level


def centred(own_key, extent, deviation, bound, shards=(), kind=jnp.bfloat16):
    result = jax.random.normal(own_key, extent, jnp.float32) * deviation
    if len(shards) > 0:
        result = block_levels(own_key, extent, shards, -0.22, 0.18) * result
    return jnp.clip(result, min=-bound, max=bound).astype(kind)


def setup_inputs(seed: int = 0, part: int = 0) -> dict:
    arg_keys = jax.random.split(jax.random.key(seed), 12)
    part_keys = jax.random.split(jax.random.fold_in(arg_keys[11], part), 12)
    queries = draw_queries(jax.random.fold_in(jax.random.fold_in(arg_keys[11], part), 71), part)
    keys = draw_keys(jax.random.fold_in(jax.random.fold_in(arg_keys[11], part), 71), part)
    values = centred(part_keys[2], (TOKENS, KV * HD), 1.0, 6.0, ((0, 4),))
    query_gain = draw_query_gain(jax.random.fold_in(arg_keys[11], 71), part)
    key_gain = draw_key_gain(jax.random.fold_in(arg_keys[11], 71), part)
    out_weight = centred(arg_keys[5], (HQ * HD, D), 0.4, 6.0)
    residual_in = centred(part_keys[6], (TOKENS, D), 1.0, 6.0, ((0, 16),))
    norm_gain = jnp.clip(1.0 + 0.18 * jax.random.normal(arg_keys[7], (D,), jnp.float32), 0.1, 1.9)
    gate_weight = centred(arg_keys[8], (D, FF), D ** -0.5, 0.125, ((0, 4), (1, 4)))
    up_weight = centred(arg_keys[9], (D, FF), D ** -0.5, 0.125, ((0, 4), (1, 4)))
    down_weight = centred(arg_keys[10], (FF, D), FF ** -0.5, 0.109375, ((0, 4), (1, 4)))
    return {"queries": queries, "keys": keys, "values": values, "query_gain": query_gain, "key_gain": key_gain, "out_weight": out_weight, "residual_in": residual_in, "norm_gain": norm_gain, "gate_weight": gate_weight, "up_weight": up_weight, "down_weight": down_weight}


def rotate(widened, positions):
    half = HD // 2
    inverse = 10000.0 ** (-jnp.arange(0, half, 2, dtype=jnp.float32) / half)
    grid_row = (positions // GRID_W).astype(jnp.float32)
    grid_col = (positions % GRID_W).astype(jnp.float32)
    angles = jnp.concatenate([grid_row[:, None] * inverse[None], grid_col[:, None] * inverse[None]], axis=-1)
    cosine = jnp.cos(angles)[:, None, :]
    sine = jnp.sin(angles)[:, None, :]
    pairs = widened.reshape(widened.shape[0], widened.shape[1], half, 2)
    first = pairs[..., 0]
    second = pairs[..., 1]
    turned = jnp.stack([first * cosine - second * sine, first * sine + second * cosine], axis=-1)
    return turned.reshape(widened.shape)

def prepare(source, gain, positions, heads):
    widened = source.astype(jnp.float32).reshape(source.shape[0], heads, HD)
    widened = widened * lax.rsqrt(lax.optimization_barrier(jnp.mean(widened * widened, axis=-1, keepdims=True)) + 1e-06) * gain
    return rotate(widened, positions).astype(jnp.bfloat16)

def reference(queries, keys, values, query_gain, key_gain, out_weight, residual_in, norm_gain, gate_weight, up_weight, down_weight):
    positions = jnp.arange(TOKENS, dtype=jnp.int32)
    query_rot = prepare(queries, query_gain, positions, HQ).transpose(1, 0, 2)
    key_rot = prepare(keys, key_gain, positions, KV).transpose(1, 0, 2)
    value_heads = values.reshape(TOKENS, KV, HD).transpose(1, 0, 2)
    group = HQ // KV
    scale = HD ** (-0.5)

    def one_head(head):
        key_block = key_rot[head // group]
        value_block = value_heads[head // group]
        query_blocks = query_rot[head].reshape(TOKENS // TOK_DEV, TOK_DEV, HD)

        def one_block(query_block):
            scores = jnp.dot(query_block, key_block.T, preferred_element_type=jnp.float32) * scale
            peak = lax.optimization_barrier(jnp.max(scores, axis=1, keepdims=True))
            raised = jnp.exp(scores - peak)
            denominator = lax.optimization_barrier(jnp.sum(raised, axis=1, keepdims=True))
            probs = raised.astype(jnp.bfloat16)
            mixed = jnp.dot(probs, value_block, preferred_element_type=jnp.float32)
            return (mixed / denominator).astype(jnp.bfloat16)
        return lax.map(one_block, query_blocks).reshape(TOKENS, HD)
    attended = lax.map(one_head, jnp.arange(HQ, dtype=jnp.int32))
    attended = attended.transpose(1, 0, 2).reshape(TOKENS, HQ * HD)
    middle = residual_in.astype(jnp.float32) + jnp.dot(attended, out_weight, preferred_element_type=jnp.float32)
    normed = middle * lax.rsqrt(lax.optimization_barrier(jnp.mean(middle * middle, axis=-1, keepdims=True)) + 1e-06) * norm_gain
    normed = normed.astype(jnp.bfloat16)
    gate_act = jnp.dot(normed, gate_weight, preferred_element_type=jnp.float32)
    up_act = jnp.dot(normed, up_weight, preferred_element_type=jnp.float32)
    hidden = (jax.nn.silu(gate_act) * up_act).astype(jnp.bfloat16)
    mixer_out = jnp.dot(hidden, down_weight, preferred_element_type=jnp.float32)
    return (middle + mixer_out).astype(jnp.bfloat16)
```

```python
import functools

import jax
import jax.numpy as jnp
from jax import lax
from jax.experimental import pallas as pl
from jax.experimental.pallas import tpu as pltpu
from jax.sharding import PartitionSpec as P

HQ = 8
KV = 2
HD = 128
GRID_W = 64
F32 = jnp.float32
BF16 = jnp.bfloat16


def lane_tables(index, gain, is_row):
    half = HD // 2
    inverse = 10000.0 ** (-jnp.arange(0, half, 2, dtype=F32) / half)
    angle = index.astype(F32)[:, None] * inverse[None]
    cosine = jnp.repeat(jnp.cos(angle), 2, axis=1)
    sine = jnp.repeat(jnp.sin(angle), 2, axis=1)
    sign = jnp.where(jnp.arange(half) % 2 == 0, -1.0, 1.0).astype(F32)
    swapped = gain.reshape(half, 2)[:, ::-1].reshape(HD)
    side = slice(0, half) if is_row else slice(half, HD)
    cosine = cosine * gain[side]
    sine = sine * sign * swapped[side]
    pad = ((0, 0), (0, half)) if is_row else ((0, 0), (half, 0))
    return jnp.pad(cosine, pad), jnp.pad(sine, pad)


def turn(raw, cos_row, sin_row, cos_col, sin_col, swap):
    rows = raw.shape[0]
    g = rows // GRID_W
    wide = raw.astype(F32)
    other = jnp.dot(raw, swap, preferred_element_type=F32)
    scale = lax.rsqrt(jnp.mean(wide * wide, axis=-1, keepdims=True) + 1e-06)
    cosine = (cos_row[:, None, :] + cos_col[None]).reshape(rows, HD)
    sine = (sin_row[:, None, :] + sin_col[None]).reshape(rows, HD)
    return ((wide * cosine + other * sine) * scale).astype(BF16)


def attend_kernel(tile, chunk, q_ref, own_ref, mine_ref, theirs_ref, qrow_ref, qcol_ref,
                  krow_ref, kcol_ref, swap_ref, out_ref, k_scr, v_scr):
    swap = swap_ref[...]

    @pl.when(pl.program_id(0) + pl.program_id(1) == 0)
    def _():
        base = 0
        for ref in (own_ref, mine_ref, theirs_ref):
            length = ref.shape[0]

            def part(i, carry, ref=ref, base=base):
                at = pl.multiple_of(i * 512, 512)
                to = pl.multiple_of(base + i * 512, 512)
                g0 = pl.multiple_of(base // GRID_W + i * 8, 8)
                k_scr[pl.ds(to, 512), :] = turn(
                    ref[pl.ds(at, 512), :HD],
                    krow_ref[0, pl.ds(g0, 8), :], krow_ref[1, pl.ds(g0, 8), :],
                    kcol_ref[0], kcol_ref[1], swap)
                v_scr[pl.ds(to, 512), :] = ref[pl.ds(at, 512), HD:]
                return carry

            lax.fori_loop(0, length // 512, part, 0)
            base += length

    gq = tile // GRID_W
    q0 = pl.program_id(1) * gq
    query = turn(q_ref[...], qrow_ref[0, pl.ds(q0, gq), :], qrow_ref[1, pl.ds(q0, gq), :],
                 qcol_ref[0], qcol_ref[1], swap)
    total = k_scr.shape[0]
    count = total // chunk
    factor = (HD ** -0.5) * 1.4426950408889634

    def scores_of(i):
        at = i * chunk if isinstance(i, int) else pl.multiple_of(i * chunk, chunk)
        return lax.dot_general(query, k_scr[pl.ds(at, chunk), :], (((1,), (1,)), ((), ())),
                               preferred_element_type=F32)

    def step(i, scores, state):
        peak, den, acc = state
        at = i * chunk if isinstance(i, int) else pl.multiple_of(i * chunk, chunk)
        new = jnp.maximum(peak, jnp.max(scores, axis=1, keepdims=True))
        keep = jnp.exp2((peak - new) * factor)
        raised = jnp.exp2((scores - new) * factor)
        den = den * keep + jnp.sum(raised, axis=1, keepdims=True)
        acc = acc * keep + jnp.dot(raised.astype(BF16), v_scr[pl.ds(at, chunk), :],
                                   preferred_element_type=F32)
        return new, den, acc

    state = (jnp.full((tile, 1), -1e30, F32), jnp.zeros((tile, 1), F32), jnp.zeros((tile, HD), F32))
    if count <= 8:
        scores = scores_of(0)
        for i in range(count):
            later = scores_of(i + 1) if i + 1 < count else None
            state = step(i, scores, state)
            scores = later
    else:
        state = lax.fori_loop(0, count, lambda i, s: step(i, scores_of(i), s), state)
    out_ref[...] = (state[2] / state[1]).astype(BF16)


def attend(queries, own, mine, theirs, qrow, qcol, krow, kcol, swap):
    rows, width = queries.shape
    heads = width // HD
    total = own.shape[0] + mine.shape[0] + theirs.shape[0]
    tile = 256
    chunk = 1024
    whole = lambda a: pl.BlockSpec(a.shape, lambda h, i: (0,) * a.ndim)
    block = pl.BlockSpec((tile, HD), lambda h, i: (i, h))
    return pl.pallas_call(
        functools.partial(attend_kernel, tile, chunk),
        grid=(heads, rows // tile),
        in_specs=[block] + [whole(a) for a in (own, mine, theirs, qrow, qcol, krow, kcol, swap)],
        out_specs=block,
        out_shape=jax.ShapeDtypeStruct((rows, width), BF16),
        scratch_shapes=[pltpu.VMEM((total, HD), BF16), pltpu.VMEM((total, HD), BF16)],
        compiler_params=pltpu.CompilerParams(
            dimension_semantics=("arbitrary", "arbitrary"), vmem_limit_bytes=56 * 2**20),
        cost_estimate=pl.CostEstimate(
            flops=rows * heads * total * HD * 8, bytes_accessed=2 * total * HD * 4,
            transcendentals=rows * heads * total),
    )(queries, own, mine, theirs, qrow, qcol, krow, kcol, swap)


def arrivals(n):
    table = []
    for z in range(n):
        here = []
        for t in range(1, n):
            if z - t >= 0:
                here.append(("R", t, z - t))
            if z + t < n:
                here.append(("L", t, z + t))
        table.append(here)
    return table


def local(n_sp, n_grp, n_tp, queries, keys, values, query_gain, key_gain, out_weight, residual_in,
          norm_gain, gate_weight, up_weight, down_weight):
    tok_rows = queries.shape[0]
    heads_here = queries.shape[1] // HD
    z = lax.axis_index("sp")
    y = lax.axis_index("grp")
    me = lax.axis_index("tp")
    core = me % 2
    n_x = n_tp // 2
    swap_core = [(i, i ^ 1) for i in range(n_tp)]

    def over_core(a):
        return lax.ppermute(a, "tp", swap_core)

    def over_x(a, d):
        return lax.ppermute(a, "tp", [(i, (i + 2 * d) % n_tp) for i in range(n_tp)])

    pair = me * heads_here // (HQ // KV)
    own_kv = jnp.concatenate(
        [lax.dynamic_slice_in_dim(a, pair * HD, HD, 1) for a in (keys, values)], axis=1)
    half = tok_rows // 2
    my_half = lax.dynamic_slice_in_dim(own_kv, core * half, half, 0)
    mine = jnp.concatenate(
        [lax.ppermute(my_half, "sp", [(i, (i + r) % n_sp) for i in range(n_sp)])
         for r in range(1, n_sp)], axis=0)
    theirs = over_core(mine)
    per = tok_rows // GRID_W
    own_rows = z * per + jnp.arange(per)
    source = ((z - 1 - jnp.arange(n_sp - 1)) % n_sp)[:, None]
    inner = jnp.arange(per // 2)[None]
    mine_rows = (source * per + core * (per // 2) + inner).reshape(-1)
    theirs_rows = (source * per + (1 - core) * (per // 2) + inner).reshape(-1)
    columns = jnp.arange(GRID_W)
    qrow = jnp.stack(lane_tables(own_rows, query_gain, True))
    qcol = jnp.stack(lane_tables(columns, query_gain, False))
    krow = jnp.stack(lane_tables(
        jnp.concatenate([own_rows, mine_rows, theirs_rows]), key_gain, True))
    kcol = jnp.stack(lane_tables(columns, key_gain, False))
    lane = jnp.arange(HD)
    swap = (lane[:, None] == (lane ^ 1)[None]).astype(BF16)

    table = arrivals(n_sp)
    sources = jnp.array([[s for _, _, s in here] for here in table], jnp.int32)[z]
    to_right = [(i, i + 1) for i in range(n_sp - 1)]
    to_left = [(i + 1, i) for i in range(n_sp - 1)]

    def gather(block, dim):
        part = block.shape[dim] // n_grp
        own = lax.dynamic_slice_in_dim(block, y * part, part, dim)
        moved = {("R", 0): own, ("L", 0): own}
        for t in range(1, n_sp):
            moved["R", t] = lax.ppermute(moved["R", t - 1], "sp", to_right)
            moved["L", t] = lax.ppermute(moved["L", t - 1], "sp", to_left)
        pieces = [lax.dynamic_slice_in_dim(block, (y - s) % n_grp * part, part, dim)
                  for s in range(n_grp)]
        for slot in range(n_sp - 1):
            piece = None
            for pos in range(n_sp):
                way, t, _ = table[pos][slot]
                piece = moved[way, t] if piece is None else jnp.where(z == pos, moved[way, t], piece)
            pieces.append(piece)
            for s in range(1, n_grp):
                pieces.append(lax.ppermute(
                    piece, "grp", [(i, (i + s) % n_grp) for i in range(n_grp)]))
        return jnp.concatenate(pieces, axis=dim)

    gate_up = gather(jnp.concatenate([gate_weight, up_weight], axis=1), 0)
    down = gather(down_weight, 1)
    ff = gate_weight.shape[1]

    attended = attend(queries, own_kv, mine, theirs, qrow, qcol, krow, kcol, swap)
    rows = residual_in.shape[0]
    traded = [None] * n_tp
    received = [lax.dynamic_slice_in_dim(attended, me * rows, rows, 0)]
    for d in range(1, n_tp):
        block = lax.dynamic_slice_in_dim(attended, (me + d) % n_tp * rows, rows, 0)
        received.append(lax.ppermute(block, "tp", [(i, (i + d) % n_tp) for i in range(n_tp)]))
    width = attended.shape[1]
    projected = 0.0
    joined = jnp.concatenate(received, axis=1)
    weight = jnp.concatenate(
        [lax.dynamic_slice_in_dim(out_weight, (me - d) % n_tp * width, width, 0)
         for d in range(n_tp)], axis=0)
    projected = jnp.dot(joined, weight, preferred_element_type=F32)
    middle = residual_in.astype(F32) + projected
    normed = (middle * lax.rsqrt(jnp.mean(middle * middle, axis=-1, keepdims=True) + 1e-06)
              * norm_gain).astype(BF16)

    block_cols = gate_weight.shape[0]
    part_cols = block_cols // n_grp
    order = [z] + [sources[i] for i in range(n_sp - 1)]
    normed = jnp.concatenate(
        [lax.dynamic_slice_in_dim(normed, b * block_cols + (y - s) % n_grp * part_cols, part_cols, 1)
         for b in order for s in range(n_grp)], axis=1)

    groups = [normed] + [over_x(normed, d) for d in range(1, n_x)]
    partial = {}
    for d in list(range(1, n_x)) + [0]:
        both = jnp.concatenate([groups[d], over_core(groups[d])], axis=0)
        act = jnp.dot(both, gate_up, preferred_element_type=F32)
        hidden = (jax.nn.silu(act[:, :ff]) * act[:, ff:]).astype(BF16)
        partial[d] = jnp.dot(hidden, down, preferred_element_type=F32).astype(BF16)
    mixer = None
    for d in list(range(1, n_x)) + [0]:
        summed = partial[d][:rows].astype(F32) + over_core(partial[d][rows:]).astype(F32)
        if d > 0:
            summed = over_x(summed.astype(BF16), n_x - d).astype(F32)
        mixer = summed if mixer is None else mixer + summed
    block_out = down_weight.shape[1]
    part_out = block_out // n_grp
    slot_of = jnp.argsort(jnp.stack(order))
    pieces = []
    for b in range(n_sp):
        for g in range(n_grp):
            at = slot_of[b] * block_out + (y - g) % n_grp * part_out
            pieces.append(lax.dynamic_slice_in_dim(mixer, at, part_out, 1))
    return (middle + jnp.concatenate(pieces, axis=1)).astype(BF16)


def solution(mesh):
    placed = (
        P(("grp", "sp"), "tp"),
        P(("grp", "sp"), None),
        P(("grp", "sp"), None),
        P(),
        P(),
        P(),
        P(("grp", "sp", "tp"), None),
        P(),
        P("sp", "tp"),
        P("sp", "tp"),
        P("tp", "sp"),
    )
    sizes = (mesh.shape["sp"], mesh.shape["grp"], mesh.shape["tp"])
    return jax.shard_map(
        functools.partial(local, *sizes),
        mesh=mesh, in_specs=placed, out_specs=P(("grp", "sp", "tp"), None), check_vma=False
    )
```

```python
import functools

import jax
import jax.numpy as jnp
from jax import lax
from jax.experimental import pallas as pl
from jax.experimental.pallas import tpu as pltpu
from jax.sharding import PartitionSpec as P

HQ = 8
KV = 2
HD = 128
GRID_W = 64
F32 = jnp.float32
BF16 = jnp.bfloat16


def lane_tables(index, gain, is_row):
    half = HD // 2
    inverse = 10000.0 ** (-jnp.arange(0, half, 2, dtype=F32) / half)
    angle = index.astype(F32)[:, None] * inverse[None]
    cosine = jnp.repeat(jnp.cos(angle), 2, axis=1)
    sine = jnp.repeat(jnp.sin(angle), 2, axis=1)
    sign = jnp.where(jnp.arange(half) % 2 == 0, -1.0, 1.0).astype(F32)
    swapped = gain.reshape(half, 2)[:, ::-1].reshape(HD)
    side = slice(0, half) if is_row else slice(half, HD)
    cosine = cosine * gain[side]
    sine = sine * sign * swapped[side]
    pad = ((0, 0), (0, half)) if is_row else ((0, 0), (half, 0))
    return jnp.pad(cosine, pad), jnp.pad(sine, pad)


def turn(raw, cos_row, sin_row, cos_col, sin_col, swap):
    rows = raw.shape[0]
    g = rows // GRID_W
    wide = raw.astype(F32)
    other = jnp.dot(raw, swap, preferred_element_type=F32)
    scale = lax.rsqrt(jnp.mean(wide * wide, axis=-1, keepdims=True) + 1e-06)
    cosine = (cos_row[:, None, :] + cos_col[None]).reshape(rows, HD)
    sine = (sin_row[:, None, :] + sin_col[None]).reshape(rows, HD)
    return ((wide * cosine + other * sine) * scale).astype(BF16)


def attend_kernel(tile, chunk, q_ref, qrow_ref, qcol_ref, krow_ref, kcol_ref, swap_ref, *refs):
    *kv_refs, out_ref, k_scr, v_scr = refs
    swap = swap_ref[...]

    @pl.when(pl.program_id(0) + pl.program_id(1) == 0)
    def _():
        base = 0
        for ref in kv_refs:
            length = ref.shape[0]

            def part(i, carry, ref=ref, base=base):
                at = pl.multiple_of(i * 512, 512)
                to = pl.multiple_of(base + i * 512, 512)
                g0 = pl.multiple_of(base // GRID_W + i * 8, 8)
                k_scr[pl.ds(to, 512), :] = turn(
                    ref[pl.ds(at, 512), :HD],
                    krow_ref[0, pl.ds(g0, 8), :], krow_ref[1, pl.ds(g0, 8), :],
                    kcol_ref[0], kcol_ref[1], swap)
                v_scr[pl.ds(to, 512), :] = ref[pl.ds(at, 512), HD:]
                return carry

            lax.fori_loop(0, length // 512, part, 0)
            base += length

    gq = tile // GRID_W
    q0 = pl.program_id(1) * gq
    query = turn(q_ref[...], qrow_ref[0, pl.ds(q0, gq), :], qrow_ref[1, pl.ds(q0, gq), :],
                 qcol_ref[0], qcol_ref[1], swap)
    total = k_scr.shape[0]
    count = total // chunk
    factor = (HD ** -0.5) * 1.4426950408889634

    def scores_of(i):
        at = i * chunk if isinstance(i, int) else pl.multiple_of(i * chunk, chunk)
        return lax.dot_general(query, k_scr[pl.ds(at, chunk), :], (((1,), (1,)), ((), ())),
                               preferred_element_type=F32)

    def step(i, scores, state):
        peak, den, acc = state
        at = i * chunk if isinstance(i, int) else pl.multiple_of(i * chunk, chunk)
        new = jnp.maximum(peak, jnp.max(scores, axis=1, keepdims=True))
        keep = jnp.exp2((peak - new) * factor)
        raised = jnp.exp2((scores - new) * factor)
        den = den * keep + jnp.sum(raised, axis=1, keepdims=True)
        acc = acc * keep + jnp.dot(raised.astype(BF16), v_scr[pl.ds(at, chunk), :],
                                   preferred_element_type=F32)
        return new, den, acc

    state = (jnp.full((tile, 1), -1e30, F32), jnp.zeros((tile, 1), F32), jnp.zeros((tile, HD), F32))
    if count <= 8:
        scores = scores_of(0)
        for i in range(count):
            later = scores_of(i + 1) if i + 1 < count else None
            state = step(i, scores, state)
            scores = later
    else:
        state = lax.fori_loop(0, count, lambda i, s: step(i, scores_of(i), s), state)
    out_ref[...] = (state[2] / state[1]).astype(BF16)


def attend(queries, qrow, qcol, krow, kcol, swap, kv):
    rows, width = queries.shape
    heads = width // HD
    total = sum(a.shape[0] for a in kv)
    tile = 256
    chunk = 1024
    whole = lambda a: pl.BlockSpec(a.shape, lambda h, i: (0,) * a.ndim)
    block = pl.BlockSpec((tile, HD), lambda h, i: (i, h))
    return pl.pallas_call(
        functools.partial(attend_kernel, tile, chunk),
        grid=(heads, rows // tile),
        in_specs=[block] + [whole(a) for a in (qrow, qcol, krow, kcol, swap, *kv)],
        out_specs=block,
        out_shape=jax.ShapeDtypeStruct((rows, width), BF16),
        scratch_shapes=[pltpu.VMEM((total, HD), BF16), pltpu.VMEM((total, HD), BF16)],
        compiler_params=pltpu.CompilerParams(
            dimension_semantics=("arbitrary", "arbitrary"), vmem_limit_bytes=56 * 2**20),
        cost_estimate=pl.CostEstimate(
            flops=rows * heads * total * HD * 8, bytes_accessed=2 * total * HD * 4,
            transcendentals=rows * heads * total),
    )(queries, qrow, qcol, krow, kcol, swap, *kv)


def local(n_sp, n_grp, n_tp, queries, keys, values, query_gain, key_gain, out_weight, residual_in,
          norm_gain, gate_weight, up_weight, down_weight):
    tok_rows = queries.shape[0]
    heads_here = queries.shape[1] // HD
    z = lax.axis_index("sp")
    y = lax.axis_index("grp")
    me = lax.axis_index("tp")
    core = me % 2
    n_x = n_tp // 2
    swap_core = [(i, i ^ 1) for i in range(n_tp)]

    def over_core(a):
        return lax.ppermute(a, "tp", swap_core)

    def over_sp(a, r):
        return lax.ppermute(a, "sp", [(i, i ^ r) for i in range(n_sp)])

    def over_x(a, d):
        return lax.ppermute(a, "tp", [(i, (i + 2 * d) % n_tp) for i in range(n_tp)])

    pair = me * heads_here // (HQ // KV)
    own_kv = jnp.concatenate(
        [lax.dynamic_slice_in_dim(a, pair * HD, HD, 1) for a in (keys, values)], axis=1)
    half = tok_rows // 2
    my_half = lax.dynamic_slice_in_dim(own_kv, core * half, half, 0)
    mine = [over_sp(my_half, r) for r in range(1, n_sp)]
    theirs = [over_core(a) for a in mine]
    per = tok_rows // GRID_W
    own_rows = z * per + jnp.arange(per)
    inner = jnp.arange(per // 2)
    mine_rows = [(z ^ r) * per + core * (per // 2) + inner for r in range(1, n_sp)]
    theirs_rows = [(z ^ r) * per + (1 - core) * (per // 2) + inner for r in range(1, n_sp)]
    columns = jnp.arange(GRID_W)
    qrow = jnp.stack(lane_tables(own_rows, query_gain, True))
    qcol = jnp.stack(lane_tables(columns, query_gain, False))
    krow = jnp.stack(lane_tables(
        jnp.concatenate([own_rows, *mine_rows, *theirs_rows]), key_gain, True))
    kcol = jnp.stack(lane_tables(columns, key_gain, False))
    lane = jnp.arange(HD)
    swap = (lane[:, None] == (lane ^ 1)[None]).astype(BF16)

    def parts_of(block, dim):
        part = block.shape[dim] // n_grp
        return [lax.dynamic_slice_in_dim(block, (y - s) % n_grp * part, part, dim)
                for s in range(n_grp)]

    def fetch(own):
        if n_sp != 4:
            return [over_sp(own, r) for r in range(1, n_sp)]
        two = over_sp(own, 2)
        one = over_sp(own, 1)
        near = lax.ppermute(own, "sp", [(1, 2), (2, 1)])
        far = lax.ppermute(two, "sp", [(1, 0), (2, 3)])
        return [one, two, jnp.where((z == 1) | (z == 2), near, far)]

    def trade(piece):
        return [piece] + [
            lax.ppermute(piece, "grp", [(i, (i + s) % n_grp) for i in range(n_grp)])
            for s in range(1, n_grp)]

    gu_parts = parts_of(jnp.concatenate([gate_weight, up_weight], axis=1), 0)
    gu_slots = fetch(gu_parts[0])
    gate_up = jnp.concatenate(
        gu_parts + [p for slot in gu_slots for p in trade(slot)], axis=0)
    down_parts = parts_of(down_weight, 1)
    down_first, _ = lax.optimization_barrier((down_parts[0], gu_slots[n_sp // 2 - 1]))
    down = [down_parts] + [trade(slot) for slot in fetch(down_first)]
    last = n_sp - 1
    down = [jnp.concatenate([p for slot in down[:last] for p in slot], axis=1),
            jnp.concatenate(down[last], axis=1)]
    ff = gate_weight.shape[1]

    attended = attend(queries, qrow, qcol, krow, kcol, swap, [own_kv, *mine, *theirs])
    rows = residual_in.shape[0]
    received = [lax.dynamic_slice_in_dim(attended, me * rows, rows, 0)]
    for d in range(1, n_tp):
        block = lax.dynamic_slice_in_dim(attended, (me + d) % n_tp * rows, rows, 0)
        received.append(lax.ppermute(block, "tp", [(i, (i + d) % n_tp) for i in range(n_tp)]))
    width = attended.shape[1]
    joined = jnp.concatenate(received, axis=1)
    weight = jnp.concatenate(
        [lax.dynamic_slice_in_dim(out_weight, (me - d) % n_tp * width, width, 0)
         for d in range(n_tp)], axis=0)
    projected = jnp.dot(joined, weight, preferred_element_type=F32)
    middle = residual_in.astype(F32) + projected
    normed = (middle * lax.rsqrt(jnp.mean(middle * middle, axis=-1, keepdims=True) + 1e-06)
              * norm_gain).astype(BF16)

    block_cols = gate_weight.shape[0]
    part_cols = block_cols // n_grp
    order = [z ^ r for r in range(n_sp)]
    normed = jnp.concatenate(
        [lax.dynamic_slice_in_dim(normed, b * block_cols + (y - s) % n_grp * part_cols, part_cols, 1)
         for b in order for s in range(n_grp)], axis=1)

    groups = [normed] + [over_x(normed, d) for d in range(1, n_x)]
    hidden = {}
    far_first = list(range(1, n_x)) + [0]
    for d in far_first:
        both = jnp.concatenate([groups[d], over_core(groups[d])], axis=0)
        act = jnp.dot(both, gate_up, preferred_element_type=F32)
        hidden[d] = (jax.nn.silu(act[:, :ff]) * act[:, ff:]).astype(BF16)
    mixed = []
    for piece in down:
        mixer = None
        for d in far_first:
            partial = jnp.dot(hidden[d], piece, preferred_element_type=F32).astype(BF16)
            summed = partial[:rows].astype(F32) + over_core(partial[rows:]).astype(F32)
            if d > 0:
                summed = over_x(summed.astype(BF16), n_x - d).astype(F32)
            mixer = summed if mixer is None else mixer + summed
        mixed.append(mixer)
    mixer = jnp.concatenate(mixed, axis=1)
    block_out = down_weight.shape[1]
    part_out = block_out // n_grp
    pieces = []
    for b in range(n_sp):
        for g in range(n_grp):
            at = (z ^ b) * block_out + (y - g) % n_grp * part_out
            pieces.append(lax.dynamic_slice_in_dim(mixer, at, part_out, 1))
    return (middle + jnp.concatenate(pieces, axis=1)).astype(BF16)


def solution(mesh):
    placed = (
        P(("grp", "sp"), "tp"),
        P(("grp", "sp"), None),
        P(("grp", "sp"), None),
        P(),
        P(),
        P(),
        P(("grp", "sp", "tp"), None),
        P(),
        P("sp", "tp"),
        P("sp", "tp"),
        P("tp", "sp"),
    )
    sizes = (mesh.shape["sp"], mesh.shape["grp"], mesh.shape["tp"])
    return jax.shard_map(
        functools.partial(local, *sizes),
        mesh=mesh, in_specs=placed, out_specs=P(("grp", "sp", "tp"), None), check_vma=False
    )
```
